32 devices in a mesh: sp: 16 (over z, y, x), tp: 2 (over core).
Axes of the slice: x: 2, y: 2, z: 4, core: 2. Of those that a mesh axis runs over, the one named last changes fastest.
Arguments:
- resid: bfloat16 [6144, 2048], P(('sp', 'tp')), may hold values from -6 to 6
- q_small: bfloat16 [6144, 1024], P('sp', 'tp'), may hold values from -6 to 6
- k_small: bfloat16 [6144, 1024], P('sp', 'tp'), may hold values from -6 to 6
- v_small: bfloat16 [6144, 1024], P('sp', 'tp'), may hold values from -6 to 6
- q_large: bfloat16 [6144, 1024], P('sp', 'tp'), may hold values from -6 to 6
- k_large: bfloat16 [6144, 1024], P('sp', 'tp'), may hold values from -6 to 6
- v_large: bfloat16 [6144, 1024], P('sp', 'tp'), may hold values from -6 to 6
- gate_small: bfloat16 [6144, 1024], P('sp', 'tp'), may hold values from -6 to 6
- large_head_gate: bfloat16 [6144, 1024], P('sp', 'tp'), may hold values from -6 to 6
- gates_small: float32 [6144, 3, 16], P('sp', None, 'tp'), may hold values from -6 to 300, as said below
- gates_large: float32 [6144, 3, 8], P('sp', None, 'tp'), may hold values from -6 to 300, as said below
- w_out_small: bfloat16 [1024, 2048], P('tp'), may hold values from -0.125 to 0.125
- w_out_large: bfloat16 [1024, 2048], P('tp'), may hold values from -0.125 to 0.125
- norm_gain: float32 [2048], replicated, may hold values from 0.1 to 1.9
- expert_ids: int32 [6144, 2], P(('sp', 'tp')), may hold values from 0 to 15, all different within a row; in each aligned block of 192 rows (0 to 191, 192 to 383, ...) at most 48 rows name the same one
- expert_weight: float32 [6144, 2], P(('sp', 'tp')), may hold values from 0.2 to 1
- w_gate: bfloat16 [16, 2048, 2048], P('sp', None, 'tp'), may hold values from -0.125 to 0.125
- w_up: bfloat16 [16, 2048, 2048], P('sp', None, 'tp'), may hold values from -0.125 to 0.125
- w_down: bfloat16 [16, 2048, 2048], P('sp', 'tp'), may hold values from -0.125 to 0.125
Outputs:
- layer_out: bfloat16 [6144, 2048], P(('sp', 'tp'))
The draws below stay inside these ranges and needn't reach their ends.
Inputs may be any that keep to these rules, and one draw needn't show every extreme that they name: `gates_small`: field 0 is the input gate's pre-activation, field 1 the forget gate's pre-activation, field 2 a non-positive term added to the log forget gate. `gates_large`: field 0 is the input gate's pre-activation, field 1 the forget gate's pre-activation, field 2 a non-positive term added to the log forget gate. `expert_ids`: each row names 2 different experts. In the 192 rows of one device no expert is named by more than 48 rows, and in some device's rows an expert is named exactly 48 times.
All inputs are finite; a program needn't handle non-finite values.
Results may differ from the reference program's by a relative error of at most 0.014.
Values may be sent and summed in bfloat16 or wider, within the bound.
A program may use at most 128 MiB of HBM per device.

```python
import math
import jax
import jax.numpy as jnp
import numpy as np
from jax import lax

D = 2048
HS = 16
DS = 64
HL = 8
DL = 128
FFE = 2048
TOPK = 2
TOK_DEV = 384
ROWS = 192
STEP_COUNT = 6144
EXPERTS = 16
CAP = 48
N_SP = 16
N_TP = 2


def gate_fields(key, head_count):
    concurrent_lanes = jax.random.split(key, 8)
    program_lattice_extent = (STEP_COUNT, head_count)
    log_in = jnp.clip(jax.random.normal(concurrent_lanes[0], program_lattice_extent), -6.0, 6.0)
    fast_share = 0.5
    is_fast = jax.random.uniform(concurrent_lanes[3], (head_count,)) < fast_share
    fast_rate = 1.0 / max(TOK_DEV // 12, 2)
    slow_rate = 0.3 / STEP_COUNT
    base_rate = jnp.where(is_fast, fast_rate, slow_rate)
    block_factor = jnp.exp(jax.random.uniform(concurrent_lanes[4], (STEP_COUNT // TOK_DEV, head_count), minval=-0.7, maxval=0.7))
    block_factor = jnp.repeat(block_factor, TOK_DEV, axis=0)
    noise = jax.random.uniform(concurrent_lanes[5], program_lattice_extent, minval=-1.0, maxval=1.0)
    rate = base_rate[None, :] * block_factor * jnp.exp(noise)
    forget_pre = -jnp.log(jnp.expm1(rate))
    packet_clusters = jax.random.uniform(concurrent_lanes[6], program_lattice_extent) < 4.0 / STEP_COUNT
    discarded_entries = jnp.log(jax.random.uniform(concurrent_lanes[7], program_lattice_extent, minval=0.5, maxval=0.8))
    surplus_quantity = jnp.where(packet_clusters, discarded_entries, 0.0)
    return jnp.stack([log_in, forget_pre, surplus_quantity], axis=1).astype(jnp.float32)


def draw_gates_small(key, part):
    return gate_fields(jax.random.fold_in(key, 11), HS)


def draw_gates_large(key, part):
    return gate_fields(jax.random.fold_in(key, 23), HL)


def block_scale(own_key, shape, cuts, least, top_value):
    level, own = 1.0, jax.random.fold_in(own_key, 6)
    for dim, parts in cuts:
        heights = jnp.exp(jax.random.uniform(jax.random.fold_in(own, dim), (parts,), jnp.float32, least / len(cuts), top_value / len(cuts)))
        level = level * jnp.repeat(heights, shape[dim] // parts).reshape([-1 if axis == dim else 1 for axis in range(len(shape))])
    return level


def routed_block(rng, own, number, rows, count, top, bound, slope):
    order = jax.random.permutation(rng, count)
    heavy_load, ordinary = portions_of(count, rows * top, bound, slope, True), portions_of(count, rows * top, bound, slope, False)
    places = jnp.arange(count)

    def named(lengths, turn):
        used = int((lengths > 0).sum())
        fixed = max(1, used // 4)
        moved = fixed + (places - fixed + turn * (used - fixed)) % max(1, count - fixed)
        return jnp.zeros((count,), jnp.int32).at[order[jnp.where(places < fixed, places, moved)]].set(jnp.asarray(lengths, jnp.int32))

    lengths = jnp.where(number % 4 == 0, named(heavy_load, number // 4), named(ordinary, number - number // 4 - 1))
    mixed = jax.random.permutation(jax.random.fold_in(own, 3), count)
    donor, taker = mixed[0:count // 2 * 2:2], mixed[1:count // 2 * 2:2]
    room = jnp.minimum(lengths[donor] - 1, bound - lengths[taker]) // 2
    room = jnp.where((donor == order[0]) | (taker == order[0]) | (lengths[taker] == 0), 0, jnp.maximum(room, 0))
    moved = jax.random.randint(jax.random.fold_in(own, 4), (count // 2,), 0, 1 << 20) % (room + 1)
    lengths = lengths.at[donor].add(-moved).at[taker].add(moved)
    members = jnp.searchsorted(jnp.cumsum(lengths), jnp.arange(rows * top), side="right").astype(jnp.int32)
    table = members.reshape(top, rows).T
    table = table[jax.random.permutation(jax.random.fold_in(own, 1), rows)]
    turn = jax.random.randint(jax.random.fold_in(own, 2), (rows, 1), 0, top)
    return jnp.take_along_axis(table, (jnp.arange(top)[None, :] + turn) % top, axis=1)


def portions_of(count, total, limit, skew, full):
    portions = [(1 << 20) // math.isqrt(grade ** skew) + 1 for grade in range(1, count + 1)]
    largest = limit if full else min(limit, max(-(-total // count), total * portions[0] // sum(portions)))
    least = 1 if total - largest >= count - 1 else 0
    given, spare = [largest] + [least] * (count - 1), total - largest - least * (count - 1)
    while spare > 0:
        movable = [i for i in range(1, count) if given[i] < largest] or [i for i in range(1, count) if given[i] < limit]
        pool, budget = sum([portions[i] for i in movable]), spare
        for i in movable:
            extra = min(limit - given[i], max(1, budget * portions[i] // pool), spare)
            given[i] = given[i] + extra
            spare = spare - extra
    return np.array(given)


def bell_draw(rng, shape, deviation, reach, pieces=(), held_as=jnp.bfloat16):
    values = jax.random.normal(rng, shape, jnp.float32) * deviation
    if len(pieces) > 0:
        values = block_scale(rng, shape, pieces, -0.22, 0.18) * values
    return jnp.clip(values, min=-reach, max=reach).astype(held_as)


def setup_inputs(seed: int = 0) -> dict:
    key_of = jax.random.split(jax.random.key(seed), 20)
    resid = bell_draw(key_of[0], (STEP_COUNT, D), 1.0, 6.0, ((0, 32),))
    q_small = bell_draw(key_of[1], (STEP_COUNT, HS * DS), 1.0, 6.0, ((0, 16), (1, 2)))
    k_small = bell_draw(key_of[2], (STEP_COUNT, HS * DS), 1.0, 6.0, ((0, 16), (1, 2)))
    v_small = bell_draw(key_of[3], (STEP_COUNT, HS * DS), 1.0, 6.0, ((0, 16), (1, 2)))
    q_large = bell_draw(key_of[4], (STEP_COUNT, HL * DL), 1.0, 6.0, ((0, 16), (1, 2)))
    k_large = bell_draw(key_of[5], (STEP_COUNT, HL * DL), 1.0, 6.0, ((0, 16), (1, 2)))
    v_large = bell_draw(key_of[6], (STEP_COUNT, HL * DL), 1.0, 6.0, ((0, 16), (1, 2)))
    gate_small = bell_draw(key_of[7], (STEP_COUNT, HS * DS), 1.5, 6.0, ((0, 16), (1, 2)))
    large_head_gate = bell_draw(key_of[8], (STEP_COUNT, HL * DL), 1.5, 6.0, ((0, 16), (1, 2)))
    gates_small = draw_gates_small(jax.random.fold_in(key_of[19], 71), 0)
    gates_large = draw_gates_large(jax.random.fold_in(key_of[19], 71), 0)
    w_out_small = bell_draw(key_of[11], (HS * DS, D), (HS * DS + HL * DL) ** -0.5, 0.125, ((0, 2),))
    w_out_large = bell_draw(key_of[12], (HL * DL, D), (HS * DS + HL * DL) ** -0.5, 0.125, ((0, 2),))
    norm_gain = jnp.clip(1.0 + 0.18 * jax.random.normal(key_of[13], (D,), jnp.float32), 0.1, 1.9)
    expert_ids_keys = jax.random.split(jax.random.fold_in(key_of[14], 1), STEP_COUNT // ROWS)
    expert_ids_turns = jax.random.permutation(jax.random.fold_in(key_of[14], 3), STEP_COUNT // ROWS)
    expert_ids = jax.vmap(lambda own, number: routed_block(jax.random.fold_in(key_of[14], 2), own, number, ROWS, EXPERTS, TOPK, CAP, 1))(expert_ids_keys, expert_ids_turns).reshape((STEP_COUNT, TOPK))
    expert_weight = jnp.clip(0.2 + 0.8 * jax.random.uniform(key_of[15], (STEP_COUNT, TOPK), jnp.float32) ** block_scale(key_of[15], (STEP_COUNT, TOPK), ((0, 32),), -0.2, 0.2), 0.2, 1.0)
    w_gate = bell_draw(key_of[16], (EXPERTS, D, FFE), D ** -0.5, 0.125, ((0, 16), (2, 2)))
    w_up = bell_draw(key_of[17], (EXPERTS, D, FFE), D ** -0.5, 0.125, ((0, 16), (2, 2)))
    w_down = bell_draw(key_of[18], (EXPERTS, FFE, D), FFE ** -0.5, 0.125, ((0, 16), (1, 2)))
    return dict(resid=resid, q_small=q_small, k_small=k_small, v_small=v_small, q_large=q_large, k_large=k_large, v_large=v_large, gate_small=gate_small, large_head_gate=large_head_gate, gates_small=gates_small, gates_large=gates_large, w_out_small=w_out_small, w_out_large=w_out_large, norm_gain=norm_gain, expert_ids=expert_ids, expert_weight=expert_weight, w_gate=w_gate, w_up=w_up, w_down=w_down)


floor_neg = -1e+30
norm_eps = 1e-06

def summarize(keys_block, values_block, log_in, log_forget):
    cumulative = jnp.cumsum(log_forget, axis=0)
    totals = cumulative[-1]
    growth = totals[None, :] - cumulative + log_in
    peak_log = lax.optimization_barrier(jnp.max(growth, axis=0))
    factor = jnp.exp(growth - peak_log[None, :])
    scaled = factor[:, :, None] * keys_block.astype(jnp.float32)
    keyed_rows = lax.optimization_barrier(scaled.astype(jnp.bfloat16)).astype(jnp.float32)
    state_mat = jnp.einsum('lhd,lhe->hde', keyed_rows, values_block.astype(jnp.float32))
    state_vec = lax.optimization_barrier(jnp.sum(scaled, axis=0))
    return (state_mat, state_vec, peak_log, totals)

def combine(earlier, later):
    earlier_mat, earlier_vec, earlier_peak, earlier_total = earlier
    later_mat, later_vec, later_peak, later_total = later
    joined = jnp.maximum(earlier_peak + later_total, later_peak)
    earlier_weight = jnp.exp(earlier_peak + later_total - joined)
    later_weight = jnp.exp(later_peak - joined)
    return (earlier_weight[:, None, None] * earlier_mat + later_weight[:, None, None] * later_mat, earlier_weight[:, None] * earlier_vec + later_weight[:, None] * later_vec, joined, earlier_total + later_total)

def read_block(queries, keys_block, values_block, log_in, log_forget, carried):
    state_mat, state_vec, carry_peak, carry_total = carried
    length = queries.shape[0]
    scaling = queries.shape[2] ** (-0.5)
    cumulative = jnp.cumsum(log_forget, axis=0).T
    entries = log_in.T
    positions = jnp.arange(length)
    causal = positions[:, None] >= positions[None, :]
    dlog = jnp.where(causal[None], cumulative[:, :, None] - cumulative[:, None, :] + entries[:, None, :], floor_neg)
    carried_log = cumulative + carry_peak[:, None]
    ceiling = jnp.maximum(carried_log, lax.optimization_barrier(jnp.max(dlog, axis=2)))
    products = jnp.einsum('thd,shd->hts', queries.astype(jnp.float32), keys_block.astype(jnp.float32)) * scaling
    scored = products * jnp.exp(dlog - ceiling[:, :, None])
    scored_b = lax.optimization_barrier(scored.astype(jnp.bfloat16)).astype(jnp.float32)
    carry_weight = jnp.exp(carried_log - ceiling)
    scaled_queries = queries.astype(jnp.float32) * scaling
    numerator = jnp.einsum('hts,shd->htd', scored_b, values_block.astype(jnp.float32))
    numerator = numerator + carry_weight[:, :, None] * jnp.einsum('thd,hde->hte', scaled_queries, state_mat, precision=lax.Precision.HIGHEST)
    denominator = lax.optimization_barrier(jnp.sum(scored, axis=2)) + carry_weight * jnp.einsum('thd,hd->ht', scaled_queries, state_vec, precision=lax.Precision.HIGHEST)
    memory = numerator / jnp.maximum(jnp.abs(denominator), 1.0)[:, :, None]
    return jnp.transpose(memory, (1, 0, 2))

def mix_group(queries, keys, values, out_gate, gates):
    head_count = gates.shape[2]
    head_dim = queries.shape[1] // head_count
    blocks = queries.shape[0] // TOK_DEV
    block_shape = (blocks, TOK_DEV, head_count, head_dim)
    log_in = gates[:, 0, :].reshape(blocks, TOK_DEV, head_count)
    log_forget = (jax.nn.log_sigmoid(gates[:, 1, :]) + gates[:, 2, :]).reshape(blocks, TOK_DEV, head_count)
    initial = (jnp.zeros((head_count, head_dim, head_dim), jnp.float32), jnp.zeros((head_count, head_dim), jnp.float32), jnp.full((head_count,), floor_neg, jnp.float32), jnp.zeros((head_count,), jnp.float32))

    def advance(carried, inputs):
        query_block, key_block, value_block, log_entry, log_keep = inputs
        memory = read_block(query_block, key_block, value_block, log_entry, log_keep, carried)
        return (combine(carried, summarize(key_block, value_block, log_entry, log_keep)), memory)
    _, memory = lax.scan(advance, initial, (queries.reshape(block_shape), keys.reshape(block_shape), values.reshape(block_shape), log_in, log_forget))
    memory = memory.reshape(queries.shape[0], head_count * head_dim)
    return (jax.nn.sigmoid(out_gate.astype(jnp.float32)) * memory).astype(jnp.bfloat16)

def expert_rows(arrived, gate_w, up_w, down_w):
    part_width = gate_w.shape[1] // N_TP
    running = jnp.zeros((arrived.shape[0], down_w.shape[1]), jnp.float32)
    for member in range(N_TP):
        low = member * part_width
        gated = jnp.dot(arrived, gate_w[:, low:low + part_width], preferred_element_type=jnp.float32)
        lifted = jnp.dot(arrived, up_w[:, low:low + part_width], preferred_element_type=jnp.float32)
        hidden = (jax.nn.silu(gated) * lifted).astype(jnp.bfloat16)
        portion = jnp.dot(hidden, down_w[low:low + part_width], preferred_element_type=jnp.float32).astype(jnp.bfloat16)
        running = running + lax.optimization_barrier(portion).astype(jnp.float32)
    return running.astype(jnp.bfloat16)

def reference(resid, q_small, k_small, v_small, q_large, k_large, v_large, gate_small, large_head_gate, gates_small, gates_large, w_out_small, w_out_large, norm_gain, expert_ids, expert_weight, w_gate, w_up, w_down):
    small_out = mix_group(q_small, k_small, v_small, gate_small, gates_small)
    large_out = mix_group(q_large, k_large, v_large, large_head_gate, gates_large)
    small_part = small_out.shape[1] // N_TP
    large_part = large_out.shape[1] // N_TP
    mixed = jnp.zeros((resid.shape[0], resid.shape[1]), jnp.float32)
    for member in range(N_TP):
        low_small = member * small_part
        low_large = member * large_part
        portion = jnp.dot(small_out[:, low_small:low_small + small_part], w_out_small[low_small:low_small + small_part], preferred_element_type=jnp.float32)
        portion = portion + jnp.dot(large_out[:, low_large:low_large + large_part], w_out_large[low_large:low_large + large_part], preferred_element_type=jnp.float32)
        mixed = mixed + lax.optimization_barrier(portion.astype(jnp.bfloat16)).astype(jnp.float32)
    after_mix = resid.astype(jnp.float32) + mixed
    normed = (after_mix * lax.rsqrt(lax.optimization_barrier(jnp.mean(after_mix * after_mix, axis=-1, keepdims=True)) + norm_eps) * norm_gain).astype(jnp.bfloat16)
    sources = N_SP * N_TP
    per_source = ROWS * TOPK
    routed = expert_ids.reshape(sources, per_source).astype(jnp.int32)
    onehot = (routed[:, :, None] == jnp.arange(EXPERTS, dtype=jnp.int32)[None, None, :]).astype(jnp.int32)
    position = lax.optimization_barrier(jnp.sum((jnp.cumsum(onehot, axis=1) - 1) * onehot, axis=2)).astype(jnp.int32)
    route_ids = jnp.arange(sources * per_source, dtype=jnp.int32).reshape(sources, per_source)
    column = jnp.arange(sources, dtype=jnp.int32)[:, None] * CAP + position
    slot_table = jnp.full((EXPERTS, sources * CAP), -1, jnp.int32).at[routed, column].set(route_ids)
    flat_weight = expert_weight.reshape(-1)

    def serve_expert(running, inputs):
        slot_row, gate_w, up_w, down_w = inputs
        filled = slot_row >= 0
        route_id = jnp.where(filled, slot_row, 0)
        token_id = route_id // TOPK
        answer = expert_rows(normed[token_id], gate_w, up_w, down_w).astype(jnp.float32)
        weight = jnp.where(filled, flat_weight[route_id], jnp.zeros((), jnp.float32))
        return (running.at[token_id].add(answer * weight[:, None]), None)
    combined, _ = lax.scan(serve_expert, jnp.zeros(after_mix.shape, jnp.float32), (slot_table, w_gate, w_up, w_down))
    return (after_mix + combined).astype(jnp.bfloat16)
```

```python
import functools

import jax
import jax.numpy as jnp
from jax import lax
from jax.experimental import pallas as pl
from jax.experimental.pallas import tpu as pltpu
from jax.sharding import PartitionSpec as P

floor_neg = -1e30
norm_eps = 1e-06
LANES = 128
MESH = pl.DeviceIdType.MESH
F32 = jnp.float32
BF16 = jnp.bfloat16


def iota(shape, axis):
    return lax.broadcasted_iota(jnp.int32, shape, axis)


def dot(a, b, ca=1, cb=0, **kw):
    return lax.dot_general(
        a, b, (((ca,), (cb,)), ((), ())), preferred_element_type=F32, **kw
    )


def exact_dot(a, b):
    return dot(a, b, precision=lax.Precision.HIGHEST)


def mixer_part(
    dims, opened,
    gates, ks, vs, kl, vl, qs, ql, gs_far, gl_far, ws_far, wl_far, resid_far, gain,
    after_ref, out_ref, ws, wl, resid, psend, precv, y,
    gs, gl,
    tot_c, tot_a, give_c, got_c, got_a, sum_c, sum_a, past_c, past_a, lead_c, pre_c, pre_a,
    inum, imax, iden,
    lsem, s1, r1, s2, r2, s2a, r2a, s3, r3, psem, rsem,
):
    planes, heads_s, heads_l = dims
    length = qs.shape[0]
    per = heads_s * LANES // qs.shape[1]
    half = LANES // per
    pairs = heads_s // per
    units = pairs + heads_l
    rows = length // 2
    me = lax.axis_index("sp")
    core = lax.axis_index("tp")
    other = 1 - core
    size = lax.axis_size("sp") // planes
    z, mine = me // size, lax.rem(me, size)
    slice_rows = tot_c.shape[0] // size

    loads = [
        pltpu.make_async_copy(src, dst, lsem.at[i])
        for i, (src, dst) in enumerate(
            ((gs_far, gs), (gl_far, gl), (ws_far, ws), (wl_far, wl), (resid_far, resid))
        )
    ]
    for load in loads:
        load.start()

    sides = [lax.rem(mine + i, size) for i in range(1, size)]
    others = [lax.rem(z + i, planes) for i in range(1, planes)]
    barrier = pltpu.get_barrier_semaphore()
    for to in [z * size + p for p in sides] + [d * size + mine for d in others]:
        pl.semaphore_signal(barrier, inc=1, device_id={"sp": to}, device_id_type=MESH)
    pl.semaphore_signal(barrier, inc=1, device_id={"tp": other}, device_id_type=MESH)

    def remote(src, dst, ssem, rsem, to):
        return pltpu.make_async_remote_copy(
            src, dst, ssem, rsem, device_id={"sp": to}, device_id_type=MESH
        )

    lane = iota((1, LANES), 1)

    def spread(columns):
        if len(columns) == 1:
            return jnp.broadcast_to(columns[0], (columns[0].shape[0], LANES))
        picked = columns[0]
        for i in range(1, len(columns)):
            picked = jnp.where(lane >= i * half, columns[i], picked)
        return picked

    def heads_of(unit):
        if unit < pairs:
            return list(range(unit * per, (unit + 1) * per))
        return [heads_s + unit - pairs]

    def view(small, large, unit):
        if unit < pairs:
            return small[:, unit * LANES : (unit + 1) * LANES]
        low = (unit - pairs) * LANES
        return large[:, low : low + LANES]

    def span(unit):
        if unit < pairs:
            return unit * half, half
        return pairs * half + (unit - pairs) * LANES, LANES

    upper_tri = (iota((length, length), 0) <= iota((length, length), 1)).astype(F32)
    lit = gates[0]
    lft = jax.nn.log_sigmoid(gates[1]) + gates[2]
    cum_row = exact_dot(lft, upper_tri)
    u_row = lit - cum_row
    cum_col = cum_row.T
    total = cum_col[length - 1 : length, :]
    grow = total - cum_col + lit.T
    peak = jnp.max(grow, axis=0, keepdims=True)
    factor = jnp.exp(grow - peak)

    for unit in range(units):
        hs = heads_of(unit)
        key = view(ks, kl, unit).astype(F32)
        scaled = spread([factor[:, h : h + 1] for h in hs]) * key
        full = dot(scaled.astype(BF16), view(vs, vl, unit), 0, 0)
        low, extent = span(unit)
        if unit < pairs:
            packed = full[:half]
            for i in range(1, per):
                packed = jnp.where(lane >= i * half, full[i * half : (i + 1) * half], packed)
        else:
            packed = full
        tot_c[low : low + extent, :] = packed
        tot_a[unit : unit + 1, :] = jnp.sum(scaled, axis=0, keepdims=True)
        tot_a[units + unit : units + unit + 1, :] = spread([peak[:, h : h + 1] for h in hs])
        tot_a[2 * units + unit : 2 * units + unit + 1, :] = spread(
            [total[:, h : h + 1] for h in hs]
        )

    def join(early, late):
        em, eb = early[units : 2 * units], early[2 * units :]
        lm, lb = late[units : 2 * units], late[2 * units :]
        m = jnp.maximum(em + lb, lm)
        ew, lw = jnp.exp(em + lb - m), jnp.exp(lm - m)
        n = ew * early[:units] + lw * late[:units]
        return jnp.concatenate([n, m, eb + lb], axis=0), ew, lw

    def owned(p):
        return pl.ds(pl.multiple_of(p * slice_rows, 16), slice_rows)

    place = iota((slice_rows, units), 0) + mine * slice_rows
    unit_at = iota((slice_rows, units), 1)
    low_at = jnp.where(unit_at < pairs, unit_at * half, pairs * half + (unit_at - pairs) * LANES)
    high_at = low_at + jnp.where(unit_at < pairs, half, LANES)
    holds = ((place >= low_at) & (place < high_at)).astype(F32)

    def widen(weights):
        wide = exact_dot(holds, jnp.concatenate(weights, axis=1))
        return [wide[:, i * LANES : (i + 1) * LANES] for i in range(len(weights))]

    give_c[...] = tot_c[...].astype(BF16)
    got_c[mine] = give_c[owned(mine), :]
    got_a[mine] = tot_a[...]
    none_a = jnp.concatenate(
        [
            jnp.zeros((units, LANES), F32),
            jnp.full((units, LANES), floor_neg, F32),
            jnp.zeros((units, LANES), F32),
        ],
        axis=0,
    )
    for d in range(planes):

        @pl.when(z <= d)
        def _():
            past_c[d] = jnp.zeros_like(past_c[d])
            past_a[d] = none_a

    def first(p):
        to = z * size + p
        return (
            remote(give_c.at[owned(p)], got_c.at[mine], s1.at[0], r1.at[0], to),
            remote(tot_a, got_a.at[mine], s1.at[1], r1.at[1], to),
        )

    def second(d):
        to = d * size + mine
        return (
            remote(sum_c, past_c.at[z], s2.at[d], r2.at[z], to),
            remote(sum_a, past_a.at[z], s2a.at[d], r2a.at[z], to),
        )

    def reached(d):
        return (
            remote(sum_c, past_c.at[d], s2.at[d], r2.at[d], me),
            remote(sum_a, past_a.at[d], s2a.at[d], r2a.at[d], me),
        )

    def third(j):
        return remote(
            lead_c.at[j], pre_c.at[owned(mine)], s3.at[0], r3.at[0], z * size + j
        )

    crowd = pl.ds(0, size - 1)
    firsts = (
        remote(got_c.at[crowd], got_c.at[crowd], s1.at[0], r1.at[0], me),
        remote(got_a.at[crowd], got_a.at[crowd], s1.at[1], r1.at[1], me),
    )
    thirds = remote(lead_c.at[crowd], lead_c.at[crowd], s3.at[0], r3.at[0], me)

    block = LANES

    def inner(unit):
        hs = heads_of(unit)
        scale = (half if unit < pairs else LANES) ** (-0.5)
        q, k, v = view(qs, ql, unit), view(ks, kl, unit), view(vs, vl, unit)
        for start in range(0, length, block):
            width = start + block
            causal = iota((block, width), 1) <= iota((block, width), 0) + start
            nums, tops, dens = [], [], []
            for i, h in enumerate(hs):
                q_block = q[start : start + block]
                if len(hs) > 1:
                    mine = (lane >= i * half) & (lane < (i + 1) * half)
                    q_block = jnp.where(mine, q_block, jnp.zeros_like(q_block))
                raw = dot(q_block, k[:width], 1, 1) * scale
                masked = jnp.where(causal, u_row[h : h + 1, :width], floor_neg)
                top = jnp.max(masked, axis=1, keepdims=True)
                scored = raw * jnp.exp(masked - top)
                dens.append(jnp.sum(scored, axis=1, keepdims=True))
                tops.append(top)
                nums.append(dot(scored.astype(BF16), v[:width]))
            num = nums[0]
            for i in range(1, len(hs)):
                num = jnp.where(lane >= i * half, nums[i], num)
            inum[unit, start : start + block, :] = num
            imax[unit, start : start + block, :] = spread(tops)
            iden[unit, start : start + block, :] = spread(dens)

    pl.semaphore_wait(barrier, len(sides) + len(others) + 1)
    for p in sides:
        for copy in first(p):
            copy.start()
    opened()
    for unit in range(pairs):
        inner(unit)
    for copy in firsts:
        copy.wait_recv()
    blocks = [got_a[i] for i in range(size)]
    whole, weights = blocks[0], [jnp.ones((units, LANES), F32)]
    for i in range(1, size):
        whole, ew, lw = join(whole, blocks[i])
        weights = [w * ew for w in weights] + [lw]
    total_c = 0.0
    for i, w in enumerate(widen(weights)):
        total_c = total_c + w * got_c[i].astype(F32)
    sum_c[...] = total_c.astype(BF16)
    sum_a[...] = whole
    for d in range(planes):

        @pl.when(d > z)
        def _():
            for copy in second(d):
                copy.start()

    for unit in range(pairs, units):
        inner(unit)
    for d in range(planes):

        @pl.when(d < z)
        def _():
            for copy in reached(d):
                copy.wait_recv()

    lead_a, weights = none_a, []
    for d in range(planes):
        lead_a, ew, lw = join(lead_a, past_a[d])
        weights = [w * ew for w in weights] + [lw]
    leads, steps = [lead_a], []
    for j in range(size - 1):
        lead_a, ew, lw = join(lead_a, blocks[j])
        leads.append(lead_a)
        steps += [ew, lw]
    wide = widen(weights + steps)
    state_c = 0.0
    for d in range(planes):
        state_c = state_c + wide[d] * past_c[d].astype(F32)
    for j in range(size):
        lead_c[j] = state_c.astype(BF16)

        @pl.when(j != mine)
        def _():
            third(j).start()

        @pl.when(j == mine)
        def _():
            pre_c[owned(mine), :] = lead_c[j]
            pre_a[...] = leads[j]

        if j < size - 1:
            ew, lw = wide[planes + 2 * j : planes + 2 * j + 2]
            state_c = ew * state_c + lw * got_c[j].astype(F32)
    for load in loads:
        load.wait()
    thirds.wait_recv()

    for unit in range(units):
        hs = heads_of(unit)
        scale = (half if unit < pairs else LANES) ** (-0.5)
        low, extent = span(unit)
        q = view(qs, ql, unit)
        state = pre_c[low : low + extent, :]
        if unit < pairs:
            state = jnp.concatenate(
                [
                    jnp.where((lane >= i * half) & (lane < (i + 1) * half), state, jnp.zeros_like(state))
                    for i in range(per)
                ],
                axis=0,
            )
        inter = dot(q, state) * scale
        qn = q.astype(F32) * pre_a[unit : unit + 1, :]
        if len(hs) > 1:
            parts = [
                jnp.sum(
                    jnp.where((lane >= i * half) & (lane < (i + 1) * half), qn, 0.0),
                    axis=1,
                    keepdims=True,
                )
                for i in range(per)
            ]
        else:
            parts = [jnp.sum(qn, axis=1, keepdims=True)]
        inter_den = spread(parts) * scale
        carry_m = pre_a[units + unit : units + unit + 1, :]
        top = jnp.maximum(carry_m, imax[unit])
        own_w, carry_w = jnp.exp(imax[unit] - top), jnp.exp(carry_m - top)
        numer = own_w * inum[unit] + carry_w * inter
        denom = own_w * iden[unit] + carry_w * inter_den
        memory = numer / jnp.maximum(jnp.abs(denom), 1.0)
        gate = jax.nn.sigmoid(view(gs, gl, unit).astype(F32))
        gated = (gate * memory).astype(BF16)
        for i in range(2):
            at = i * units * LANES + unit * LANES
            y[:, at : at + LANES] = gated[i * rows : (i + 1) * rows]

    cut = qs.shape[1]
    features = ws.shape[1]
    step_n = 512

    def project(which, n):
        low = pl.multiple_of(which * (units * LANES), LANES)
        left = y[:, pl.ds(low, cut)]
        right = y[:, pl.ds(low + cut, units * LANES - cut)]
        at = (slice(None), slice(n, n + step_n))
        return (dot(left, ws[at]) + dot(right, wl[at])).astype(BF16)

    def swap(n):
        at = (slice(None), pl.ds(n, step_n))
        i = n // step_n
        return pltpu.make_async_remote_copy(
            psend.at[at], precv.at[at], psem.at[i], rsem.at[i],
            device_id={"tp": other}, device_id_type=MESH,
        )

    for n in range(0, features, step_n):
        psend[:, n : n + step_n] = project(other, n)
        swap(n).start()
    power = 0.0
    for n in range(0, features, step_n):
        at = (slice(None), slice(n, n + step_n))
        own = project(core, n).astype(F32)
        swap(n).wait_recv()
        after = resid[at].astype(F32) + (own + precv[at].astype(F32))
        after_ref[at] = after
        power = power + jnp.sum(after * after, axis=-1, keepdims=True)
    scale = lax.rsqrt(power * (1.0 / features) + norm_eps)
    for n in range(0, features, step_n):
        at = (slice(None), slice(n, n + step_n))
        out_ref[at] = (after_ref[at] * scale * gain[:, n : n + step_n]).astype(BF16)

    for copy in firsts:
        copy.wait_send()
    for d in range(planes):

        @pl.when(d > z)
        def _():
            for copy in second(d):
                copy.wait_send()

    thirds.wait_send()
    for n in range(0, features, step_n):
        swap(n).wait_send()


def orders(planes):
    centre = (planes - 1) / 2

    def order(z):
        rank = lambda d: (abs(d - z), 0 if (d > z) == (z < centre) else 1)
        return sorted(range(planes), key=rank)

    return [order(z) for z in range(planes)]


def schedule(planes):
    none = -1
    order = orders(planes)
    last = planes + 1
    names = ("work", "next", "also", "mid", "join", "late", "tail")
    rows = {name: [] for name in names}
    for z in range(planes):
        o = order[z]
        plan = [dict.fromkeys(rows, none) for _ in range(last + 1)]
        plan[0].update(next=o[1])
        if z in (0, planes - 1):
            plan[1].update(work=o[1], mid=o[2], join=o[1])
            plan[2].update(work=o[2], mid=o[3], join=o[2])
            plan[3].update(work=o[3], join=o[3])
            plan[4].update(work=o[0])
            plan[5].update(late=o[0])
        else:
            plan[0].update(also=o[2])
            plan[1].update(work=o[1], mid=o[3])
            plan[2].update(work=o[2])
            plan[3].update(work=o[3])
            plan[4].update(work=o[0], join=o[1])
            plan[5].update(join=o[3], tail=o[2], late=o[0])
        for name in rows:
            rows[name].append([step[name] for step in plan])
    return rows, last + 1


def experts_part(
    capacity, planes, loaded, normed, ids, wts, out_ref,
    wg, wu, wd, acc, disp, psend, hidden, ret,
    all_ids, all_wts, sel, comb, tok, arr, pin,
    ids_s, ids_r, wts_s, wts_r, tok_s, tok_r, dis_s, dis_r, ret_s, ret_r, pin_s, pin_r,
):
    peers = lax.axis_size("sp")
    me = lax.axis_index("sp")
    size = peers // planes
    z, mine = me // size, lax.rem(me, size)
    part, features = wd.shape[0] // 2, wd.shape[1]
    rows = normed.shape[0]
    slots = size * capacity
    tile = 512
    chunks = features // tile

    def remote(src, dst, ssem, rsem, to):
        return pltpu.make_async_remote_copy(
            src, dst, ssem, rsem, device_id={"sp": to}, device_id_type=MESH
        )

    def sent(ref, sem):
        return remote(ref, ref, sem, sem, me)

    sides = [lax.rem(mine + i, size) for i in range(1, size)]
    others = [lax.rem(z + i, planes) for i in range(1, planes)]

    def row(d):
        return pl.ds(pl.multiple_of(d * rows, 16), rows)

    def slot(d, p=0, count=slots):
        return pl.ds(pl.multiple_of(d * slots + p * capacity, 16), count)

    def cols(c):
        if isinstance(c, int):
            return pl.ds(c * tile, tile)
        return pl.ds(pl.multiple_of(c * tile, tile), tile)

    def block(p):
        return pl.ds(pl.multiple_of(p * capacity, 16), capacity)

    def tell(d, at):
        to = d * size + mine
        return (
            remote(ids, all_ids.at[at], ids_s.at[d], ids_r.at[at], to),
            remote(wts, all_wts.at[at], wts_s.at[d], wts_r.at[at], to),
        )

    def own_up(c):
        return remote(
            normed.at[:, cols(c)], tok.at[z, :, cols(c)], tok_s.at[z], tok_r.at[z, c],
            me + size,
        )

    def own_down(c):
        return remote(
            normed.at[:, cols(c)], tok.at[z, :, cols(c)], tok_s.at[planes], tok_r.at[z, c],
            me - size,
        )

    def relay(d, c, to):
        return remote(
            tok.at[d, :, cols(c)], tok.at[d, :, cols(c)], tok_s.at[d], tok_r.at[d, c], to
        )

    for d in others:
        for copy in tell(d, z):
            copy.start()
    for c in range(chunks):

        @pl.when(z < planes - 1)
        def _():
            own_up(c).start()

        @pl.when(z > 0)
        def _():
            own_down(c).start()

    all_ids[z] = ids[...]
    all_wts[z] = wts[...]
    tok[z] = normed[...]

    pad = size + -size % 16

    def route(d):
        @pl.when(d != z)
        def _():
            for copy in tell(d, d):
                copy.wait_recv()

        names, shares = all_ids[d], all_wts[d]
        expert = iota((pad, rows), 0) + z * size
        first, second = names[0:1, :] == expert, names[1:2, :] == expert
        hit = (first | second).astype(BF16)
        weight = jnp.where(first, shares[0:1, :], 0.0) + jnp.where(second, shares[1:2, :], 0.0)
        before = (iota((rows, rows), 0) < iota((rows, rows), 1)).astype(BF16)
        count = dot(hit, before)
        number = iota((slots, 1), 0).astype(F32)
        group = jnp.floor((number + 0.5) * (1.0 / capacity))
        place = number - group * capacity
        member = (group == iota((slots, pad), 1).astype(F32)).astype(BF16)
        chosen = (dot(member, hit) > 0.5) & (dot(member, count.astype(BF16)) == place)
        sel[d] = chosen.astype(BF16)
        comb[d] = jnp.where(chosen, dot(member, weight.astype(BF16)), 0.0).astype(BF16)

    many = len(sides) * capacity
    crowd = pl.ds(0, many)

    def dispatch(d, c, p):
        return remote(
            disp.at[slot(d, p, capacity), cols(c)], arr.at[d, block(mine), cols(c)],
            dis_s.at[d], dis_r.at[d, c], z * size + p,
        )

    def dispatched(d, c):
        at = arr.at[d, crowd, cols(c)]
        return remote(at, at, dis_s.at[d], dis_r.at[d, c], me)

    def answer(d, c, p):
        return remote(
            disp.at[slot(d, p, capacity), cols(c)], ret.at[d, block(mine), cols(c)],
            ret_s.at[d], ret_r.at[d, c], z * size + p,
        )

    def answered(d, c):
        at = ret.at[d, crowd, cols(c)]
        return remote(at, at, ret_s.at[d], ret_r.at[d, c], me)

    def partial(d, c, at, to):
        return remote(
            psend.at[row(d), cols(c)], pin.at[at, :, cols(c)],
            pin_s.at[d], pin_r.at[at, c], to,
        )

    def forward(d, c):
        @pl.when(d != z)
        def _():
            relay(d, c, me).wait_recv()

        @pl.when((d < z) & (z < planes - 1))
        def _():
            relay(d, c, me + size).start()

        @pl.when((d > z) & (z > 0))
        def _():
            relay(d, c, me - size).start()

    def lift(d, c):
        disp[slot(d), cols(c)] = dot(sel[d], tok[d, :, cols(c)]).astype(BF16)
        for p in sides:
            dispatch(d, c, p).start()

    def work(d):
        arr[d, block(mine), :] = disp[slot(d, mine, capacity), :]
        for c in range(chunks):
            dispatched(d, c).wait_recv()
        for side in range(2):

            def up(n, carry):
                at = cols(n)
                x = arr[d]
                gated = dot(x, wg[side, :, at])
                lifted = dot(x, wu[side, :, at])
                to = pl.ds(pl.multiple_of(side * part + n * tile, tile), tile)
                hidden[:, to] = (gated * jax.nn.sigmoid(gated) * lifted).astype(BF16)
                return carry

            lax.fori_loop(0, part // tile, up, 0)

    def finish(d):
        sent(disp.at[slot(d, 0, many)], dis_s.at[d]).wait_send()

        def lower(c, carry):
            disp[slot(d), cols(c)] = dot(hidden[...], wd[:, cols(c)]).astype(BF16)
            for p in sides:
                answer(d, c, p).start()
            return carry

        lax.fori_loop(0, chunks, lower, 0)
        ret[d, block(mine), :] = disp[slot(d, mine, capacity), :]

    def join(d, c):
        answered(d, c).wait_recv()
        at = cols(c)

        def own():
            return dot(comb[d], ret[d, :, at], 0, 0)

        above, below = d > z, d < z
        inner = (above & (z > 0)) | (below & (z < planes - 1))

        @pl.when(d == z)
        def _():
            acc[:, at] = acc[:, at] + own()

        @pl.when(inner)
        def _():
            partial(d, c, d, me).wait_recv()
            psend[row(d), at] = (own() + pin[d, :, at].astype(F32)).astype(BF16)

        @pl.when((d != z) & jnp.logical_not(inner))
        def _():
            psend[row(d), at] = own().astype(BF16)

        @pl.when(above)
        def _():
            partial(d, c, d, me + size).start()

        @pl.when(below)
        def _():
            partial(d, c, jnp.where(d == z - 1, planes, d), me - size).start()

    table, count = schedule(planes)

    def pick(name, step):
        found = jnp.int32(-1)
        for zz, entries in enumerate(table[name]):
            for i, value in enumerate(entries):
                if value >= 0:
                    found = jnp.where((z == zz) & (step == i), value, found)
        return found

    def turn(step, carry):
        busy, then, second = pick("work", step), pick("next", step), pick("also", step)
        mid, soon = pick("mid", step), pick("join", step)
        late, tail = pick("late", step), pick("tail", step)
        half = chunks // 2

        @pl.when(step == 1)
        def _():
            loaded()

        @pl.when(mid >= 0)
        def _():
            route(mid)
            forward(mid, 0)
            lift(mid, 0)

        @pl.when((mid >= 0) & (step == 2))
        def _():
            for c in range(1, half):
                forward(mid, c)
                lift(mid, c)

        @pl.when(busy >= 0)
        def _():
            work(busy)

        @pl.when(then >= 0)
        def _():
            route(then)
            for c in range(chunks):
                forward(then, c)

                @pl.when(second >= 0)
                def _():
                    forward(second, c)

                lift(then, c)

        @pl.when(second >= 0)
        def _():
            route(second)
            for c in range(chunks):
                lift(second, c)

        @pl.when((mid >= 0) & (step != 2))
        def _():
            for c in range(1, half):
                forward(mid, c)
                lift(mid, c)

        @pl.when((mid >= 0) & (step == 2))
        def _():
            forward(mid, half)
            lift(mid, half)

        @pl.when(busy >= 0)
        def _():
            finish(busy)

        @pl.when((mid >= 0) & (step != 2))
        def _():
            forward(mid, half)
            lift(mid, half)

        @pl.when((soon >= 0) & (step == 1))
        def _():
            join(soon, 0)

        @pl.when(mid >= 0)
        def _():
            for c in range(half + 1, chunks):
                forward(mid, c)
                lift(mid, c)

        lag = 2
        for c in range(chunks + lag):
            if c < chunks:

                @pl.when((soon >= 0) & jnp.logical_not((step == 1) & (c == 0)))
                def _():
                    join(soon, c)

            if c >= lag:

                @pl.when(tail >= 0)
                def _():
                    join(tail, c - lag)

        @pl.when(late >= 0)
        def _():
            for c in range(chunks):
                join(late, c)

        return carry

    route(z)
    for c in range(chunks):
        lift(z, c)
    lax.fori_loop(0, count, turn, 0)

    @pl.when(z < planes - 1)
    def _():
        sent(tok.at[z], tok_s.at[z]).wait_send()

    @pl.when(z > 0)
    def _():
        sent(tok.at[z], tok_s.at[planes]).wait_send()

    for c in range(chunks):
        at = cols(c)

        @pl.when(z > 0)
        def _():
            partial(z, c, z, me).wait_recv()
            acc[:, at] = acc[:, at] + pin[z, :, at].astype(F32)

        @pl.when(z < planes - 1)
        def _():
            partial(z, c, planes, me).wait_recv()
            acc[:, at] = acc[:, at] + pin[planes, :, at].astype(F32)

        out_ref[:, at] = acc[:, at].astype(BF16)

    for d in others:
        for copy in tell(d, z):
            copy.wait_send()
    def drain(d, carry):
        @pl.when(((d < z) & (z < planes - 1)) | ((d > z) & (z > 0)))
        def _():
            sent(tok.at[d], tok_s.at[d]).wait_send()

        @pl.when(d != z)
        def _():
            sent(psend.at[row(d)], pin_s.at[d]).wait_send()

        sent(disp.at[slot(d, 0, many)], ret_s.at[d]).wait_send()
        return carry

    lax.fori_loop(0, planes, drain, 0)


def layer_kernel(dims, *refs):
    planes, heads_s, heads_l, capacity, counts = dims
    refs = list(refs)

    def take(n):
        found = refs[:n]
        del refs[:n]
        return found

    given, ids, wts, own_g, own_u, own_d, out_ref = take(13), *take(6)
    wg, wu, wd, acc, disp, psend, hidden, ret = take(8)
    normed = out_ref
    lsem, xs, xr = take(3)
    mix, rest = take(counts[0]), take(counts[1])
    part, rows = own_d.shape[0], normed.shape[0]
    other = 1 - lax.axis_index("tp")
    loads = [
        pltpu.make_async_copy(src, dst, lsem.at[i])
        for i, (src, dst) in enumerate(
            ((own_g, wg.at[0]), (own_u, wu.at[0]), (own_d, wd.at[pl.ds(0, part)]))
        )
    ]
    trades = [
        pltpu.make_async_remote_copy(
            src, dst, xs.at[i], xr.at[i], device_id={"tp": other}, device_id_type=MESH
        )
        for i, (src, dst) in enumerate(
            ((own_g, wg.at[1]), (own_u, wu.at[1]), (own_d, wd.at[pl.ds(part, part)]))
        )
    ]

    def opened():
        for trade in trades[:2]:
            trade.start()
        for load in loads:
            load.start()

    def loaded():
        for load in loads:
            load.wait()
        for trade in trades:
            trade.wait_recv()

    depth = given[9].shape[0]
    mixer_part(
        (planes, heads_s, heads_l), opened, *given, acc, normed,
        disp.at[pl.ds(0, depth)], psend.at[pl.ds(0, depth)], disp.at[pl.ds(depth, rows)],
        psend.at[pl.ds(depth, rows)], ret.at[0, pl.ds(0, rows)], hidden.at[pl.ds(0, rows)], *mix,
    )
    trades[2].start()
    experts_part(
        capacity, planes, loaded, normed, ids, wts, out_ref, wg, wu, wd, acc, disp, psend, hidden, ret,
        *rest,
    )
    for trade in trades:
        trade.wait_send()


def body(*args):
    (resid, qs, ks, vs, ql, kl, vl, gs, gl, gates_s, gates_l, ws, wl, gain, ids, wts) = args[:16]
    own_w = [w[0] for w in args[16:]]
    planes = 4
    experts = args[16].shape[0] * lax.axis_size("sp")
    size = lax.axis_size("sp") // planes
    capacity = max(2, qs.shape[0] * ids.shape[1] // experts)
    capacity += -capacity % 16
    slots = size * capacity
    heads_s, heads_l = gates_s.shape[2], gates_l.shape[2]
    gates = jnp.concatenate([gates_s, gates_l], axis=2)
    gates = jnp.pad(gates, ((0, 0), (0, 0), (0, -gates.shape[2] % 8)))
    gates = jnp.transpose(gates, (1, 2, 0))
    ids, wts = ids.T, wts.T
    rows, features = resid.shape
    length = qs.shape[0]
    half = qs.shape[1] // heads_s
    pairs = qs.shape[1] // LANES
    units = pairs + heads_l
    state = pairs * half + heads_l * LANES
    part = state // size
    depth, width = own_w[0].shape
    chunks = features // 512
    vm = pl.BlockSpec(memory_space=pltpu.VMEM)
    hbm = pl.BlockSpec(memory_space=pltpu.HBM)
    vmem, dma = pltpu.VMEM, pltpu.SemaphoreType.DMA
    common = [
        vmem((2, depth, width), BF16),
        vmem((2, depth, width), BF16),
        vmem((2 * width, features), BF16),
        vmem((rows, features), F32),
        vmem((planes * slots, features), BF16),
        vmem((planes * rows, features), BF16),
        vmem((slots, 2 * width), BF16),
        vmem((planes, slots, features), BF16),
        dma((3,)),
        dma((3,)),
        dma((3,)),
    ]
    mix = [
        vmem(gs.shape, BF16),
        vmem(gl.shape, BF16),
        vmem((state, LANES), F32),
        vmem((3 * units, LANES), F32),
        vmem((state, LANES), BF16),
        vmem((size, part, LANES), BF16),
        vmem((size, 3 * units, LANES), F32),
        vmem((part, LANES), BF16),
        vmem((3 * units, LANES), F32),
        vmem((planes, part, LANES), BF16),
        vmem((planes, 3 * units, LANES), F32),
        vmem((size, part, LANES), BF16),
        vmem((state, LANES), BF16),
        vmem((3 * units, LANES), F32),
        vmem((units, length, LANES), F32),
        vmem((units, length, LANES), F32),
        vmem((units, length, LANES), F32),
        dma((5,)),
        dma((2,)),
        dma((2,)),
        dma((planes,)),
        dma((planes,)),
        dma((planes,)),
        dma((planes,)),
        dma((1,)),
        dma((1,)),
        dma((chunks,)),
        dma((chunks,)),
    ]
    rest = [
        vmem((planes,) + ids.shape, jnp.int32),
        vmem((planes,) + wts.shape, F32),
        vmem((planes, slots, rows), BF16),
        vmem((planes, slots, rows), BF16),
        vmem((planes, rows, features), BF16),
        vmem((planes, slots, features), BF16),
        vmem((planes + 1, rows, features), BF16),
        dma((planes,)),
        dma((planes,)),
        dma((planes,)),
        dma((planes,)),
        dma((planes + 1,)),
        dma((planes, chunks)),
        dma((planes,)),
        dma((planes, chunks)),
        dma((planes,)),
        dma((planes, chunks)),
        dma((planes,)),
        dma((planes + 1, chunks)),
    ]
    return pl.pallas_call(
        functools.partial(
            layer_kernel, (planes, heads_s, heads_l, capacity, (len(mix), len(rest)))
        ),
        out_shape=jax.ShapeDtypeStruct((rows, features), BF16),
        in_specs=[vm] * 7 + [hbm] * 5 + [vm] * 3 + [hbm] * 3,
        out_specs=vm,
        scratch_shapes=common + mix + rest,
        compiler_params=pltpu.CompilerParams(
            collective_id=0, has_side_effects=True, vmem_limit_bytes=67_000_000
        ),
        cost_estimate=pl.CostEstimate(
            flops=140_000_000_000, bytes_accessed=48_000_000, transcendentals=0
        ),
        name="layer",
    )(
        gates, ks, vs, kl, vl, qs, ql, gs, gl, ws, wl, resid, gain.reshape(1, -1),
        ids, wts, *own_w,
    )


def solution(mesh):
    return jax.shard_map(
        body,
        mesh=mesh,
        in_specs=(
            P(("sp", "tp"), None),
            P("sp", "tp"),
            P("sp", "tp"),
            P("sp", "tp"),
            P("sp", "tp"),
            P("sp", "tp"),
            P("sp", "tp"),
            P("sp", "tp"),
            P("sp", "tp"),
            P("sp", None, "tp"),
            P("sp", None, "tp"),
            P("tp", None),
            P("tp", None),
            P(),
            P(("sp", "tp"), None),
            P(("sp", "tp"), None),
            P("sp", None, "tp"),
            P("sp", None, "tp"),
            P("sp", "tp", None),
        ),
        out_specs=P(("sp", "tp"), None),
        check_vma=False,
    )
```

```python
import functools

import jax
import jax.numpy as jnp
from jax import lax
from jax.experimental import pallas as pl
from jax.experimental.pallas import tpu as pltpu
from jax.sharding import PartitionSpec as P

floor_neg = -1e30
norm_eps = 1e-06
LANES = 128
MESH = pl.DeviceIdType.MESH
F32 = jnp.float32
BF16 = jnp.bfloat16


def iota(shape, axis):
    return lax.broadcasted_iota(jnp.int32, shape, axis)


def dot(a, b, ca=1, cb=0, **kw):
    return lax.dot_general(
        a, b, (((ca,), (cb,)), ((), ())), preferred_element_type=F32, **kw
    )


def exact_dot(a, b):
    return dot(a, b, precision=lax.Precision.HIGHEST)


def mixer_part(
    dims, opened, leave,
    gates, ks, vs, kl, vl, qs_far, ql_far, gs_far, gl_far, ws_far, wl_far, resid_far, gain,
    after_ref, out_ref, ws, wl, resid, psend, precv, y,
    qs, ql, gs, gl,
    tot_c, tot_a, give_c, got_c, got_a, sum_c, sum_a, past_c, past_a, lead_c, pre_c, pre_a,
    inum, imax, iden,
    lsem, s1, r1, s2, r2, s2a, r2a, s3, r3, psem, rsem,
):
    planes, heads_s, heads_l = dims
    length = qs.shape[0]
    per = heads_s * LANES // qs.shape[1]
    half = LANES // per
    pairs = heads_s // per
    units = pairs + heads_l
    rows = length // 2
    me = lax.axis_index("sp")
    core = lax.axis_index("tp")
    other = 1 - core
    size = lax.axis_size("sp") // planes
    z, mine = me // size, lax.rem(me, size)
    slice_rows = tot_c.shape[0] // size

    loads = [
        pltpu.make_async_copy(src, dst, lsem.at[i])
        for i, (src, dst) in enumerate(
            (
                (qs_far, qs), (ql_far, ql), (gs_far, gs), (gl_far, gl),
                (ws_far, ws), (wl_far, wl), (resid_far, resid),
            )
        )
    ]
    for load in loads:
        load.start()

    sides = [lax.rem(mine + i, size) for i in range(1, size)]
    others = [lax.rem(z + i, planes) for i in range(1, planes)]
    barrier = pltpu.get_barrier_semaphore()
    for to in [z * size + p for p in sides] + [d * size + mine for d in others]:
        pl.semaphore_signal(barrier, inc=1, device_id={"sp": to}, device_id_type=MESH)
    pl.semaphore_signal(barrier, inc=1, device_id={"tp": other}, device_id_type=MESH)

    def remote(src, dst, ssem, rsem, to):
        return pltpu.make_async_remote_copy(
            src, dst, ssem, rsem, device_id={"sp": to}, device_id_type=MESH
        )

    lane = iota((1, LANES), 1)

    def spread(columns):
        if len(columns) == 1:
            return jnp.broadcast_to(columns[0], (columns[0].shape[0], LANES))
        picked = columns[0]
        for i in range(1, len(columns)):
            picked = jnp.where(lane >= i * half, columns[i], picked)
        return picked

    def heads_of(unit):
        if unit < pairs:
            return list(range(unit * per, (unit + 1) * per))
        return [heads_s + unit - pairs]

    def view(small, large, unit):
        if unit < pairs:
            return small[:, unit * LANES : (unit + 1) * LANES]
        low = (unit - pairs) * LANES
        return large[:, low : low + LANES]

    def span(unit):
        if unit < pairs:
            return unit * half, half
        return pairs * half + (unit - pairs) * LANES, LANES

    upper_tri = (iota((length, length), 0) <= iota((length, length), 1)).astype(F32)
    lit = gates[0]
    lft = jax.nn.log_sigmoid(gates[1]) + gates[2]
    cum_row = exact_dot(lft, upper_tri)
    u_row = lit - cum_row
    cum_col = cum_row.T
    total = cum_col[length - 1 : length, :]
    grow = total - cum_col + lit.T
    peak = jnp.max(grow, axis=0, keepdims=True)
    factor = jnp.exp(grow - peak)

    for unit in range(units):
        hs = heads_of(unit)
        key = view(ks, kl, unit).astype(F32)
        scaled = spread([factor[:, h : h + 1] for h in hs]) * key
        full = dot(scaled.astype(BF16), view(vs, vl, unit), 0, 0)
        low, extent = span(unit)
        if unit < pairs:
            packed = full[:half]
            for i in range(1, per):
                packed = jnp.where(lane >= i * half, full[i * half : (i + 1) * half], packed)
        else:
            packed = full
        tot_c[low : low + extent, :] = packed
        tot_a[unit : unit + 1, :] = jnp.sum(scaled, axis=0, keepdims=True)
        tot_a[units + unit : units + unit + 1, :] = spread([peak[:, h : h + 1] for h in hs])
        tot_a[2 * units + unit : 2 * units + unit + 1, :] = spread(
            [total[:, h : h + 1] for h in hs]
        )

    def join(early, late):
        em, eb = early[units : 2 * units], early[2 * units :]
        lm, lb = late[units : 2 * units], late[2 * units :]
        m = jnp.maximum(em + lb, lm)
        ew, lw = jnp.exp(em + lb - m), jnp.exp(lm - m)
        n = ew * early[:units] + lw * late[:units]
        return jnp.concatenate([n, m, eb + lb], axis=0), ew, lw

    def owned(p):
        return pl.ds(pl.multiple_of(p * slice_rows, 16), slice_rows)

    place = iota((slice_rows, units), 0) + mine * slice_rows
    unit_at = iota((slice_rows, units), 1)
    low_at = jnp.where(unit_at < pairs, unit_at * half, pairs * half + (unit_at - pairs) * LANES)
    high_at = low_at + jnp.where(unit_at < pairs, half, LANES)
    holds = ((place >= low_at) & (place < high_at)).astype(F32)

    def widen(weights):
        wide = exact_dot(holds, jnp.concatenate(weights, axis=1))
        return [wide[:, i * LANES : (i + 1) * LANES] for i in range(len(weights))]

    give_c[...] = tot_c[...].astype(BF16)
    got_c[mine] = give_c[owned(mine), :]
    got_a[mine] = tot_a[...]
    none_a = jnp.concatenate(
        [
            jnp.zeros((units, LANES), F32),
            jnp.full((units, LANES), floor_neg, F32),
            jnp.zeros((units, LANES), F32),
        ],
        axis=0,
    )
    for d in range(planes):

        @pl.when(z <= d)
        def _():
            past_c[d] = jnp.zeros_like(past_c[d])
            past_a[d] = none_a

    def first(p):
        to = z * size + p
        return (
            remote(give_c.at[owned(p)], got_c.at[mine], s1.at[0], r1.at[0], to),
            remote(tot_a, got_a.at[mine], s1.at[1], r1.at[1], to),
        )

    def second(d):
        to = d * size + mine
        return (
            remote(sum_c, past_c.at[z], s2.at[d], r2.at[z], to),
            remote(sum_a, past_a.at[z], s2a.at[d], r2a.at[z], to),
        )

    def reached(d):
        return (
            remote(sum_c, past_c.at[d], s2.at[d], r2.at[d], me),
            remote(sum_a, past_a.at[d], s2a.at[d], r2a.at[d], me),
        )

    def third(j):
        return remote(
            lead_c.at[j], pre_c.at[owned(mine)], s3.at[0], r3.at[0], z * size + j
        )

    crowd = pl.ds(0, size - 1)
    firsts = (
        remote(got_c.at[crowd], got_c.at[crowd], s1.at[0], r1.at[0], me),
        remote(got_a.at[crowd], got_a.at[crowd], s1.at[1], r1.at[1], me),
    )
    thirds = remote(lead_c.at[crowd], lead_c.at[crowd], s3.at[0], r3.at[0], me)

    block = LANES

    def inner(unit):
        hs = heads_of(unit)
        scale = (half if unit < pairs else LANES) ** (-0.5)
        q, k, v = view(qs, ql, unit), view(ks, kl, unit), view(vs, vl, unit)
        for start in range(0, length, block):
            width = start + block
            causal = iota((block, width), 1) <= iota((block, width), 0) + start
            nums, tops, dens = [], [], []
            for i, h in enumerate(hs):
                q_block = q[start : start + block]
                if len(hs) > 1:
                    mine = (lane >= i * half) & (lane < (i + 1) * half)
                    q_block = jnp.where(mine, q_block, jnp.zeros_like(q_block))
                raw = dot(q_block, k[:width], 1, 1) * scale
                masked = jnp.where(causal, u_row[h : h + 1, :width], floor_neg)
                top = jnp.max(masked, axis=1, keepdims=True)
                scored = raw * jnp.exp(masked - top)
                dens.append(jnp.sum(scored, axis=1, keepdims=True))
                tops.append(top)
                nums.append(dot(scored.astype(BF16), v[:width]))
            num = nums[0]
            for i in range(1, len(hs)):
                num = jnp.where(lane >= i * half, nums[i], num)
            inum[unit, start : start + block, :] = num
            imax[unit, start : start + block, :] = spread(tops)
            iden[unit, start : start + block, :] = spread(dens)

    pl.semaphore_wait(barrier, len(sides) + len(others) + 1)
    for p in sides:
        for copy in first(p):
            copy.start()
    opened()
    for load in loads[:2]:
        load.wait()
    for unit in range(pairs):
        inner(unit)
    for copy in firsts:
        copy.wait_recv()
    blocks = [got_a[i] for i in range(size)]
    whole, weights = blocks[0], [jnp.ones((units, LANES), F32)]
    for i in range(1, size):
        whole, ew, lw = join(whole, blocks[i])
        weights = [w * ew for w in weights] + [lw]
    total_c = 0.0
    for i, w in enumerate(widen(weights)):
        total_c = total_c + w * got_c[i].astype(F32)
    sum_c[...] = total_c.astype(BF16)
    sum_a[...] = whole
    for d in range(planes):

        @pl.when(d > z)
        def _():
            for copy in second(d):
                copy.start()

    for unit in range(pairs, units):
        inner(unit)
    for d in range(planes):

        @pl.when(d < z)
        def _():
            for copy in reached(d):
                copy.wait_recv()

    lead_a, weights = none_a, []
    for d in range(planes):
        lead_a, ew, lw = join(lead_a, past_a[d])
        weights = [w * ew for w in weights] + [lw]
    leads, steps = [lead_a], []
    for j in range(size - 1):
        lead_a, ew, lw = join(lead_a, blocks[j])
        leads.append(lead_a)
        steps += [ew, lw]
    wide = widen(weights + steps)
    state_c = 0.0
    for d in range(planes):
        state_c = state_c + wide[d] * past_c[d].astype(F32)
    for j in range(size):
        lead_c[j] = state_c.astype(BF16)

        @pl.when(j != mine)
        def _():
            third(j).start()

        @pl.when(j == mine)
        def _():
            pre_c[owned(mine), :] = lead_c[j]
            pre_a[...] = leads[j]

        if j < size - 1:
            ew, lw = wide[planes + 2 * j : planes + 2 * j + 2]
            state_c = ew * state_c + lw * got_c[j].astype(F32)
    for load in loads[2:]:
        load.wait()
    thirds.wait_recv()

    for unit in range(units):
        hs = heads_of(unit)
        scale = (half if unit < pairs else LANES) ** (-0.5)
        low, extent = span(unit)
        q = view(qs, ql, unit)
        state = pre_c[low : low + extent, :]
        if unit < pairs:
            state = jnp.concatenate(
                [
                    jnp.where((lane >= i * half) & (lane < (i + 1) * half), state, jnp.zeros_like(state))
                    for i in range(per)
                ],
                axis=0,
            )
        inter = dot(q, state) * scale
        qn = q.astype(F32) * pre_a[unit : unit + 1, :]
        if len(hs) > 1:
            parts = [
                jnp.sum(
                    jnp.where((lane >= i * half) & (lane < (i + 1) * half), qn, 0.0),
                    axis=1,
                    keepdims=True,
                )
                for i in range(per)
            ]
        else:
            parts = [jnp.sum(qn, axis=1, keepdims=True)]
        inter_den = spread(parts) * scale
        carry_m = pre_a[units + unit : units + unit + 1, :]
        top = jnp.maximum(carry_m, imax[unit])
        own_w, carry_w = jnp.exp(imax[unit] - top), jnp.exp(carry_m - top)
        numer = own_w * inum[unit] + carry_w * inter
        denom = own_w * iden[unit] + carry_w * inter_den
        memory = numer / jnp.maximum(jnp.abs(denom), 1.0)
        gate = jax.nn.sigmoid(view(gs, gl, unit).astype(F32))
        gated = (gate * memory).astype(BF16)
        for i in range(2):
            at = i * units * LANES + unit * LANES
            y[:, at : at + LANES] = gated[i * rows : (i + 1) * rows]

    cut = qs.shape[1]
    features = ws.shape[1]
    step_n = 512

    def project(which, n):
        low = pl.multiple_of(which * (units * LANES), LANES)
        left = y[:, pl.ds(low, cut)]
        right = y[:, pl.ds(low + cut, units * LANES - cut)]
        at = (slice(None), slice(n, n + step_n))
        return (dot(left, ws[at]) + dot(right, wl[at])).astype(BF16)

    def swap(n):
        at = (slice(None), pl.ds(n, step_n))
        i = n // step_n
        return pltpu.make_async_remote_copy(
            psend.at[at], precv.at[at], psem.at[i], rsem.at[i],
            device_id={"tp": other}, device_id_type=MESH,
        )

    for n in range(0, features, step_n):
        psend[:, n : n + step_n] = project(other, n)
        swap(n).start()
    power = 0.0
    for n in range(0, features, step_n):
        at = (slice(None), slice(n, n + step_n))
        own = project(core, n).astype(F32)
        swap(n).wait_recv()
        after = resid[at].astype(F32) + (own + precv[at].astype(F32))
        after_ref[at] = after
        power = power + jnp.sum(after * after, axis=-1, keepdims=True)
    scale = lax.rsqrt(power * (1.0 / features) + norm_eps)
    for n in range(0, features, step_n):
        at = (slice(None), slice(n, n + step_n))
        out_ref[at] = (after_ref[at] * scale * gain[:, n : n + step_n]).astype(BF16)
        leave(n // step_n)

    for copy in firsts:
        copy.wait_send()
    for d in range(planes):

        @pl.when(d > z)
        def _():
            for copy in second(d):
                copy.wait_send()

    thirds.wait_send()
    for n in range(0, features, step_n):
        swap(n).wait_send()


def orders(planes):
    centre = (planes - 1) / 2

    def order(z):
        rank = lambda d: (abs(d - z), 0 if (d > z) == (z < centre) else 1)
        return sorted(range(planes), key=rank)

    return [order(z) for z in range(planes)]


def schedule(planes):
    none = -1
    order = orders(planes)
    last = planes + 1
    names = ("work", "next", "also", "mid", "join", "late", "tail")
    rows = {name: [] for name in names}
    for z in range(planes):
        o = order[z]
        plan = [dict.fromkeys(rows, none) for _ in range(last + 1)]
        plan[0].update(next=o[1])
        if z in (0, planes - 1):
            plan[1].update(work=o[1], mid=o[2], join=o[1])
            plan[2].update(work=o[2], mid=o[3], join=o[2])
            plan[3].update(work=o[3], join=o[3])
            plan[4].update(work=o[0])
            plan[5].update(late=o[0])
        else:
            plan[0].update(also=o[2])
            plan[1].update(work=o[1], mid=o[3])
            plan[2].update(work=o[2])
            plan[3].update(work=o[3])
            plan[4].update(work=o[0], join=o[1])
            plan[5].update(join=o[3], tail=o[2], late=o[0])
        for name in rows:
            rows[name].append([step[name] for step in plan])
    return rows, last + 1


def experts_part(
    capacity, planes, loaded, normed, ids, wts, out_ref,
    wg, wu, wd, acc, disp, psend, hidden, ret,
    all_ids, all_wts, sel, comb, tok, arr, pin,
    ids_s, ids_r, wts_s, wts_r, tok_s, tok_r, dis_s, dis_r, ret_s, ret_r, pin_s, pin_r,
):
    peers = lax.axis_size("sp")
    me = lax.axis_index("sp")
    size = peers // planes
    z, mine = me // size, lax.rem(me, size)
    part, features = wd.shape[0] // 2, wd.shape[1]
    rows = normed.shape[0]
    slots = size * capacity
    tile = 512
    chunks = features // tile

    def remote(src, dst, ssem, rsem, to):
        return pltpu.make_async_remote_copy(
            src, dst, ssem, rsem, device_id={"sp": to}, device_id_type=MESH
        )

    def sent(ref, sem):
        return remote(ref, ref, sem, sem, me)

    sides = [lax.rem(mine + i, size) for i in range(1, size)]
    others = [lax.rem(z + i, planes) for i in range(1, planes)]

    def row(d):
        return pl.ds(pl.multiple_of(d * rows, 16), rows)

    def slot(d, p=0, count=slots):
        return pl.ds(pl.multiple_of(d * slots + p * capacity, 16), count)

    def cols(c):
        if isinstance(c, int):
            return pl.ds(c * tile, tile)
        return pl.ds(pl.multiple_of(c * tile, tile), tile)

    def block(p):
        return pl.ds(pl.multiple_of(p * capacity, 16), capacity)

    def tell(d, at):
        to = d * size + mine
        return (
            remote(ids, all_ids.at[at], ids_s.at[d], ids_r.at[at], to),
            remote(wts, all_wts.at[at], wts_s.at[d], wts_r.at[at], to),
        )

    def relay(d, c, to):
        return remote(
            tok.at[d, :, cols(c)], tok.at[d, :, cols(c)], tok_s.at[d], tok_r.at[d, c], to
        )

    for d in others:
        for copy in tell(d, z):
            copy.start()
    all_ids[z] = ids[...]
    all_wts[z] = wts[...]
    tok[z] = normed[...]

    pad = size + -size % 16

    def route(d):
        @pl.when(d != z)
        def _():
            for copy in tell(d, d):
                copy.wait_recv()

        names, shares = all_ids[d], all_wts[d]
        expert = iota((pad, rows), 0) + z * size
        first, second = names[0:1, :] == expert, names[1:2, :] == expert
        hit = (first | second).astype(BF16)
        weight = jnp.where(first, shares[0:1, :], 0.0) + jnp.where(second, shares[1:2, :], 0.0)
        before = (iota((rows, rows), 0) < iota((rows, rows), 1)).astype(BF16)
        count = dot(hit, before)
        number = iota((slots, 1), 0).astype(F32)
        group = jnp.floor((number + 0.5) * (1.0 / capacity))
        place = number - group * capacity
        member = (group == iota((slots, pad), 1).astype(F32)).astype(BF16)
        chosen = (dot(member, hit) > 0.5) & (dot(member, count.astype(BF16)) == place)
        sel[d] = chosen.astype(BF16)
        comb[d] = jnp.where(chosen, dot(member, weight.astype(BF16)), 0.0).astype(BF16)

    many = len(sides) * capacity
    crowd = pl.ds(0, many)

    def dispatch(d, c, p):
        return remote(
            disp.at[slot(d, p, capacity), cols(c)], arr.at[d, block(mine), cols(c)],
            dis_s.at[d], dis_r.at[d, c], z * size + p,
        )

    def dispatched(d, c):
        at = arr.at[d, crowd, cols(c)]
        return remote(at, at, dis_s.at[d], dis_r.at[d, c], me)

    def answer(d, c, p):
        return remote(
            disp.at[slot(d, p, capacity), cols(c)], ret.at[d, block(mine), cols(c)],
            ret_s.at[d], ret_r.at[d, c], z * size + p,
        )

    def answered(d, c):
        at = ret.at[d, crowd, cols(c)]
        return remote(at, at, ret_s.at[d], ret_r.at[d, c], me)

    def partial(d, c, at, to):
        return remote(
            psend.at[row(d), cols(c)], pin.at[at, :, cols(c)],
            pin_s.at[d], pin_r.at[at, c], to,
        )

    def forward(d, c):
        @pl.when(d != z)
        def _():
            relay(d, c, me).wait_recv()

        @pl.when((d < z) & (z < planes - 1))
        def _():
            relay(d, c, me + size).start()

        @pl.when((d > z) & (z > 0))
        def _():
            relay(d, c, me - size).start()

    def lift(d, c):
        disp[slot(d), cols(c)] = dot(sel[d], tok[d, :, cols(c)]).astype(BF16)
        for p in sides:
            dispatch(d, c, p).start()

    def work(d):
        arr[d, block(mine), :] = disp[slot(d, mine, capacity), :]
        for c in range(chunks):
            dispatched(d, c).wait_recv()
        for side in range(2):

            def up(n, carry):
                at = cols(n)
                x = arr[d]
                gated = dot(x, wg[side, :, at])
                lifted = dot(x, wu[side, :, at])
                to = pl.ds(pl.multiple_of(side * part + n * tile, tile), tile)
                hidden[:, to] = (gated * jax.nn.sigmoid(gated) * lifted).astype(BF16)
                return carry

            lax.fori_loop(0, part // tile, up, 0)

    def finish(d):
        sent(disp.at[slot(d, 0, many)], dis_s.at[d]).wait_send()

        def lower(c, carry):
            disp[slot(d), cols(c)] = dot(hidden[...], wd[:, cols(c)]).astype(BF16)
            for p in sides:
                answer(d, c, p).start()
            return carry

        lax.fori_loop(0, chunks, lower, 0)
        ret[d, block(mine), :] = disp[slot(d, mine, capacity), :]

    def join(d, c):
        answered(d, c).wait_recv()
        at = cols(c)

        def own():
            return dot(comb[d], ret[d, :, at], 0, 0)

        above, below = d > z, d < z
        inner = (above & (z > 0)) | (below & (z < planes - 1))

        @pl.when(d == z)
        def _():
            acc[:, at] = acc[:, at] + own()

        @pl.when(inner)
        def _():
            partial(d, c, d, me).wait_recv()
            psend[row(d), at] = (own() + pin[d, :, at].astype(F32)).astype(BF16)

        @pl.when((d != z) & jnp.logical_not(inner))
        def _():
            psend[row(d), at] = own().astype(BF16)

        @pl.when(above)
        def _():
            partial(d, c, d, me + size).start()

        @pl.when(below)
        def _():
            partial(d, c, jnp.where(d == z - 1, planes, d), me - size).start()

    table, count = schedule(planes)

    def pick(name, step):
        found = jnp.int32(-1)
        for zz, entries in enumerate(table[name]):
            for i, value in enumerate(entries):
                if value >= 0:
                    found = jnp.where((z == zz) & (step == i), value, found)
        return found

    def turn(step, carry):
        busy, then, second = pick("work", step), pick("next", step), pick("also", step)
        mid, soon = pick("mid", step), pick("join", step)
        late, tail = pick("late", step), pick("tail", step)
        half = chunks // 2

        @pl.when(step == 1)
        def _():
            loaded()

        @pl.when(mid >= 0)
        def _():
            route(mid)
            forward(mid, 0)
            lift(mid, 0)

        @pl.when((mid >= 0) & (step == 2))
        def _():
            for c in range(1, half):
                forward(mid, c)
                lift(mid, c)

        @pl.when(busy >= 0)
        def _():
            work(busy)

        @pl.when(then >= 0)
        def _():
            route(then)
            for c in range(chunks):
                forward(then, c)

                @pl.when(second >= 0)
                def _():
                    forward(second, c)

                lift(then, c)

        @pl.when(second >= 0)
        def _():
            route(second)
            for c in range(chunks):
                lift(second, c)

        @pl.when((mid >= 0) & (step != 2))
        def _():
            for c in range(1, half):
                forward(mid, c)
                lift(mid, c)

        @pl.when((mid >= 0) & (step == 2))
        def _():
            forward(mid, half)
            lift(mid, half)

        @pl.when(busy >= 0)
        def _():
            finish(busy)

        @pl.when((mid >= 0) & (step != 2))
        def _():
            forward(mid, half)
            lift(mid, half)

        @pl.when((soon >= 0) & (step == 1))
        def _():
            join(soon, 0)

        @pl.when(mid >= 0)
        def _():
            for c in range(half + 1, chunks):
                forward(mid, c)
                lift(mid, c)

        lag = 2
        for c in range(chunks + lag):
            if c < chunks:

                @pl.when((soon >= 0) & jnp.logical_not((step == 1) & (c == 0)))
                def _():
                    join(soon, c)

            if c >= lag:

                @pl.when(tail >= 0)
                def _():
                    join(tail, c - lag)

        @pl.when(late >= 0)
        def _():
            for c in range(chunks):
                join(late, c)

        return carry

    route(z)
    for c in range(chunks):
        lift(z, c)
    lax.fori_loop(0, count, turn, 0)

    @pl.when(z < planes - 1)
    def _():
        sent(tok.at[z], tok_s.at[z]).wait_send()

    @pl.when(z > 0)
    def _():
        sent(tok.at[z], tok_s.at[planes]).wait_send()

    for c in range(chunks):
        at = cols(c)

        @pl.when(z > 0)
        def _():
            partial(z, c, z, me).wait_recv()
            acc[:, at] = acc[:, at] + pin[z, :, at].astype(F32)

        @pl.when(z < planes - 1)
        def _():
            partial(z, c, planes, me).wait_recv()
            acc[:, at] = acc[:, at] + pin[planes, :, at].astype(F32)

        out_ref[:, at] = acc[:, at].astype(BF16)

    for d in others:
        for copy in tell(d, z):
            copy.wait_send()
    def drain(d, carry):
        @pl.when(((d < z) & (z < planes - 1)) | ((d > z) & (z > 0)))
        def _():
            sent(tok.at[d], tok_s.at[d]).wait_send()

        @pl.when(d != z)
        def _():
            sent(psend.at[row(d)], pin_s.at[d]).wait_send()

        sent(disp.at[slot(d, 0, many)], ret_s.at[d]).wait_send()
        return carry

    lax.fori_loop(0, planes, drain, 0)


def layer_kernel(dims, *refs):
    planes, heads_s, heads_l, capacity, counts = dims
    refs = list(refs)

    def take(n):
        found = refs[:n]
        del refs[:n]
        return found

    given, ids, wts, own_g, own_u, own_d, out_ref = take(13), *take(6)
    wg, wu, wd, acc, disp, psend, hidden, ret = take(8)
    normed = out_ref
    lsem, xs, xr = take(3)
    mix, rest = take(counts[0]), take(counts[1])
    part, rows = own_d.shape[0], normed.shape[0]
    other = 1 - lax.axis_index("tp")
    loads = [
        pltpu.make_async_copy(src, dst, lsem.at[i])
        for i, (src, dst) in enumerate(
            ((own_g, wg.at[0]), (own_u, wu.at[0]), (own_d, wd.at[pl.ds(0, part)]))
        )
    ]
    trades = [
        pltpu.make_async_remote_copy(
            src, dst, xs.at[i], xr.at[i], device_id={"tp": other}, device_id_type=MESH
        )
        for i, (src, dst) in enumerate(
            ((own_g, wg.at[1]), (own_u, wu.at[1]), (own_d, wd.at[pl.ds(part, part)]))
        )
    ]

    def opened():
        for trade in trades[:2]:
            trade.start()
        for load in loads:
            load.start()

    def loaded():
        for load in loads:
            load.wait()
        for trade in trades:
            trade.wait_recv()

    tok, tok_s, tok_r = rest[4], rest[11], rest[12]
    me = lax.axis_index("sp")
    size = lax.axis_size("sp") // planes
    z = me // size

    def leave(c):
        at = (slice(None), pl.ds(c * 512, 512))

        def go(to, sem):
            pltpu.make_async_remote_copy(
                normed.at[at], tok.at[z].at[at], sem, tok_r.at[z, c],
                device_id={"sp": to}, device_id_type=MESH,
            ).start()

        @pl.when(z < planes - 1)
        def _():
            go(me + size, tok_s.at[z])

        @pl.when(z > 0)
        def _():
            go(me - size, tok_s.at[planes])

    depth = given[9].shape[0]
    mixer_part(
        (planes, heads_s, heads_l), opened, leave, *given, acc, normed,
        disp.at[pl.ds(0, depth)], psend.at[pl.ds(0, depth)], disp.at[pl.ds(depth, rows)],
        psend.at[pl.ds(depth, rows)], ret.at[0, pl.ds(0, rows)], hidden.at[pl.ds(0, rows)], *mix,
    )
    trades[2].start()
    experts_part(
        capacity, planes, loaded, normed, ids, wts, out_ref, wg, wu, wd, acc, disp, psend, hidden, ret,
        *rest,
    )
    for trade in trades:
        trade.wait_send()


def body(*args):
    (resid, qs, ks, vs, ql, kl, vl, gs, gl, gates_s, gates_l, ws, wl, gain, ids, wts) = args[:16]
    own_w = [w[0] for w in args[16:]]
    planes = 4
    experts = args[16].shape[0] * lax.axis_size("sp")
    size = lax.axis_size("sp") // planes
    capacity = max(2, qs.shape[0] * ids.shape[1] // experts)
    capacity += -capacity % 16
    slots = size * capacity
    heads_s, heads_l = gates_s.shape[2], gates_l.shape[2]
    gates = jnp.concatenate([gates_s, gates_l], axis=2)
    gates = jnp.pad(gates, ((0, 0), (0, 0), (0, -gates.shape[2] % 8)))
    gates = jnp.transpose(gates, (1, 2, 0))
    ids, wts = ids.T, wts.T
    rows, features = resid.shape
    length = qs.shape[0]
    half = qs.shape[1] // heads_s
    pairs = qs.shape[1] // LANES
    units = pairs + heads_l
    state = pairs * half + heads_l * LANES
    part = state // size
    depth, width = own_w[0].shape
    chunks = features // 512
    vm = pl.BlockSpec(memory_space=pltpu.VMEM)
    hbm = pl.BlockSpec(memory_space=pltpu.HBM)
    vmem, dma = pltpu.VMEM, pltpu.SemaphoreType.DMA
    common = [
        vmem((2, depth, width), BF16),
        vmem((2, depth, width), BF16),
        vmem((2 * width, features), BF16),
        vmem((rows, features), F32),
        vmem((planes * slots, features), BF16),
        vmem((planes * rows, features), BF16),
        vmem((slots, 2 * width), BF16),
        vmem((planes, slots, features), BF16),
        dma((3,)),
        dma((3,)),
        dma((3,)),
    ]
    mix = [
        vmem(qs.shape, BF16),
        vmem(ql.shape, BF16),
        vmem(gs.shape, BF16),
        vmem(gl.shape, BF16),
        vmem((state, LANES), F32),
        vmem((3 * units, LANES), F32),
        vmem((state, LANES), BF16),
        vmem((size, part, LANES), BF16),
        vmem((size, 3 * units, LANES), F32),
        vmem((part, LANES), BF16),
        vmem((3 * units, LANES), F32),
        vmem((planes, part, LANES), BF16),
        vmem((planes, 3 * units, LANES), F32),
        vmem((size, part, LANES), BF16),
        vmem((state, LANES), BF16),
        vmem((3 * units, LANES), F32),
        vmem((units, length, LANES), F32),
        vmem((units, length, LANES), F32),
        vmem((units, length, LANES), F32),
        dma((7,)),
        dma((2,)),
        dma((2,)),
        dma((planes,)),
        dma((planes,)),
        dma((planes,)),
        dma((planes,)),
        dma((1,)),
        dma((1,)),
        dma((chunks,)),
        dma((chunks,)),
    ]
    rest = [
        vmem((planes,) + ids.shape, jnp.int32),
        vmem((planes,) + wts.shape, F32),
        vmem((planes, slots, rows), BF16),
        vmem((planes, slots, rows), BF16),
        vmem((planes, rows, features), BF16),
        vmem((planes, slots, features), BF16),
        vmem((planes + 1, rows, features), BF16),
        dma((planes,)),
        dma((planes,)),
        dma((planes,)),
        dma((planes,)),
        dma((planes + 1,)),
        dma((planes, chunks)),
        dma((planes,)),
        dma((planes, chunks)),
        dma((planes,)),
        dma((planes, chunks)),
        dma((planes,)),
        dma((planes + 1, chunks)),
    ]
    return pl.pallas_call(
        functools.partial(
            layer_kernel, (planes, heads_s, heads_l, capacity, (len(mix), len(rest)))
        ),
        out_shape=jax.ShapeDtypeStruct((rows, features), BF16),
        in_specs=[vm] * 5 + [hbm] * 7 + [vm] * 3 + [hbm] * 3,
        out_specs=vm,
        scratch_shapes=common + mix + rest,
        compiler_params=pltpu.CompilerParams(
            collective_id=0, has_side_effects=True, vmem_limit_bytes=67_000_000
        ),
        cost_estimate=pl.CostEstimate(
            flops=140_000_000_000, bytes_accessed=48_000_000, transcendentals=0
        ),
        name="layer",
    )(
        gates, ks, vs, kl, vl, qs, ql, gs, gl, ws, wl, resid, gain.reshape(1, -1),
        ids, wts, *own_w,
    )


def solution(mesh):
    return jax.shard_map(
        body,
        mesh=mesh,
        in_specs=(
            P(("sp", "tp"), None),
            P("sp", "tp"),
            P("sp", "tp"),
            P("sp", "tp"),
            P("sp", "tp"),
            P("sp", "tp"),
            P("sp", "tp"),
            P("sp", "tp"),
            P("sp", "tp"),
            P("sp", None, "tp"),
            P("sp", None, "tp"),
            P("tp", None),
            P("tp", None),
            P(),
            P(("sp", "tp"), None),
            P(("sp", "tp"), None),
            P("sp", None, "tp"),
            P("sp", None, "tp"),
            P("sp", "tp", None),
        ),
        out_specs=P(("sp", "tp"), None),
        check_vma=False,
    )
```
